32 devices in a mesh: sp: 16 (over z, y, x), tp: 2 (over core).
Axes of the slice: x: 2, y: 2, z: 4, core: 2. Of those that a mesh axis runs over, the one named last changes fastest.
Arguments:
- query_small: bfloat16 [6144, 2, 128], P('sp', 'tp'), may hold values from -8 to 8
- key_small: bfloat16 [6144, 2, 128], P('sp', 'tp'), may hold values from -8 to 8
- value_small: bfloat16 [6144, 2, 128], P('sp', 'tp'), may hold values from -6 to 6
- query_large: bfloat16 [6144, 2, 256], P('sp', 'tp'), may hold values from -8 to 8
- key_large: bfloat16 [6144, 2, 256], P('sp', 'tp'), may hold values from -8 to 8
- value_large: bfloat16 [6144, 2, 128], P('sp', 'tp'), may hold values from -6 to 6
- lambdas: float32 [2, 2], P('tp'), may hold values from 0.3 to 0.8
- slopes: float32 [2, 2], P('tp'), as said below
- head_gain: bfloat16 [128], replicated, may hold values from 0.099609375 to 1.8984375
- residual: bfloat16 [6144, 2048], P(('sp', 'tp')), may hold values from -6 to 6
- out_weight: bfloat16 [512, 2048], replicated, may hold values from -0.25 to 0.25
- norm_gains: bfloat16 [2, 2048], replicated, may hold values from 0.099609375 to 1.8984375
- routes: int32 [6144, 2], P(('sp', 'tp')), may hold values from 0 to 15, as said below
- route_weights: float32 [6144, 2], P(('sp', 'tp')), may hold values from 0.1 to 1
- gate_weight: bfloat16 [16, 2048, 1024], P('sp', None, 'tp'), may hold values from -0.125 to 0.125
- up_weight: bfloat16 [16, 2048, 1024], P('sp', None, 'tp'), may hold values from -0.125 to 0.125
- down_weight: bfloat16 [16, 1024, 2048], P('sp', 'tp'), may hold values from -0.1875 to 0.1875
Outputs:
- layer_out: bfloat16 [6144, 2048], P(('sp', 'tp'))
The draws below stay inside these ranges and needn't reach their ends.
Inputs may be any that keep to these rules, and one draw needn't show every extreme that they name: `slopes`: positive. `routes`: each token names two different experts of one group of 4 consecutive expert numbers. In each aligned block of 192 rows (the tokens of one device) no expert is named more than 48 times, and some expert is named exactly 48 times in every block.
All inputs are finite; a program needn't handle non-finite values.
Results may differ from the reference program's by a relative error of at most 0.011.
Values may be sent and summed in bfloat16 or wider, within the bound.
A program may use at most 128 MiB of HBM per device.

```python
import math
import jax
import jax.numpy as jnp
from jax import lax

D = 2048
HG = 2
DS = 64
DL = 128
DV = 128
FF = 1024
TOPK = 2
GROUPS = 4
TOKENS = 6144
ROWS = 192
EXPERTS = 16
CAP = 48
N_TP = 2


def paired_draw(key, key_width):
    folded = jax.random.fold_in(key, 1000 + key_width)
    query_key, keyset_key = jax.random.split(folded, 2)
    spread = math.sqrt(1.75)
    queries = jnp.clip(jax.random.normal(query_key, (TOKENS, HG, 2 * key_width), jnp.float32) * spread, -8.0, 8.0)
    keyset = jnp.clip(jax.random.normal(keyset_key, (TOKENS, HG, 2 * key_width), jnp.float32) * spread, -8.0, 8.0)
    return (queries, keyset)


def draw_query_small(key, part):
    return paired_draw(key, DS)[0].astype(jnp.bfloat16)


def draw_key_small(key, part):
    return paired_draw(key, DS)[1].astype(jnp.bfloat16)


def draw_query_large(key, part):
    return paired_draw(key, DL)[0].astype(jnp.bfloat16)


def draw_key_large(key, part):
    return paired_draw(key, DL)[1].astype(jnp.bfloat16)


def draw_slopes(key, part):
    folded = jax.random.fold_in(key, 7)
    order_key, level_key = jax.random.split(folded)
    ranking = jax.random.permutation(order_key, 2 * HG)
    levels = jax.random.uniform(level_key, (2 * HG,), jnp.float32)
    slower = jnp.exp(math.log(0.25 / TOKENS) + levels * math.log(8.0))
    faster = jnp.exp(math.log(1.0 / 16.0) + levels * math.log(2.0))
    keeping = HG
    return jnp.where(ranking < keeping, slower, faster).reshape(HG, 2).astype(jnp.float32)


def draw_routes(key, part):
    folded = jax.random.fold_in(key, 11)
    group_key, blocks_key = jax.random.split(folded)
    group_size = EXPERTS // GROUPS
    halfway = ROWS // 2
    busiest = jax.random.randint(group_key, (), 0, GROUPS)

    def one_block(block_key):
        first_key, second_key, offset_key, permute_key, swap_key, order_key = jax.random.split(block_key, 6)
        first_cut = jax.random.randint(first_key, (), 0, halfway + 1)
        second_cut = jax.random.randint(second_key, (), 0, halfway + 1)
        lower_cut = jnp.minimum(first_cut, second_cut)
        upper_cut = jnp.maximum(first_cut, second_cut)
        others = (busiest + 1 + jnp.arange(GROUPS - 1)) % GROUPS
        counts = jnp.zeros((GROUPS,), jnp.int32).at[busiest].set(halfway)
        counts = counts.at[others].set(jnp.stack([lower_cut, upper_cut - lower_cut, halfway - upper_cut]).astype(jnp.int32))
        group_ends = jnp.cumsum(counts)
        starts = group_ends - counts
        position = jnp.arange(ROWS)
        chosen = jnp.sum((position[:, None] >= group_ends[None, :]).astype(jnp.int32), axis=1)
        within = position - starts[chosen]
        offsets = jax.random.randint(offset_key, (GROUPS,), 1, group_size)
        permuted = jax.vmap(lambda sub_key: jax.random.permutation(sub_key, group_size))(jax.random.split(permute_key, GROUPS))
        leading = permuted[chosen, within % group_size]
        trailing = permuted[chosen, (within + offsets[chosen]) % group_size]
        pair_ids = jnp.stack([leading, trailing], axis=1) + (chosen * group_size)[:, None]
        swapped = jax.random.randint(swap_key, (ROWS,), 0, 2)
        pair_ids = jnp.where(swapped[:, None] == 1, pair_ids[:, ::-1], pair_ids)
        shuffle = jax.random.permutation(order_key, ROWS)
        return pair_ids[shuffle]
    block_keys = jax.random.split(blocks_key, TOKENS // ROWS)
    return jax.vmap(one_block)(block_keys).reshape(TOKENS, 2).astype(jnp.int32)


def shard_levels(rng, dims, shards, low, top_value):
    gain, own = 1.0, jax.random.fold_in(rng, 6)
    for dim, blocks in shards:
        draws = jnp.exp(jax.random.uniform(jax.random.fold_in(own, dim), (blocks,), jnp.float32, low / len(shards), top_value / len(shards)))
        gain = gain * jnp.repeat(draws, dims[dim] // blocks).reshape([-1 if axis == dim else 1 for axis in range(len(dims))])
    return gain


def normal_values(key, shape, scale, most, cuts=(), held_as=jnp.bfloat16):
    values = scale * jax.random.normal(key, shape, jnp.float32)
    if cuts:
        values = values * shard_levels(key, shape, cuts, -0.22, 0.18)
    return jnp.clip(values, -most, most).astype(held_as)


def setup_inputs(seed: int = 0) -> dict:
    arg_keys = jax.random.split(jax.random.key(seed), 18)
    return {
        "query_small": draw_query_small(jax.random.fold_in(arg_keys[17], 71), 0),
        "key_small": draw_key_small(jax.random.fold_in(arg_keys[17], 71), 0),
        "value_small": normal_values(arg_keys[2], (TOKENS, HG, DV), 1.0, 6.0, ((0, 16), (1, 2))),
        "query_large": draw_query_large(jax.random.fold_in(arg_keys[17], 71), 0),
        "key_large": draw_key_large(jax.random.fold_in(arg_keys[17], 71), 0),
        "value_large": normal_values(arg_keys[5], (TOKENS, HG, DV), 1.0, 6.0, ((0, 16), (1, 2))),
        "lambdas": jnp.clip(0.3 + 0.5 * jax.random.uniform(arg_keys[6], (HG, 2), jnp.float32) ** shard_levels(arg_keys[6], (HG, 2), ((0, 2),), -0.2, 0.2), 0.3, 0.8),
        "slopes": draw_slopes(jax.random.fold_in(arg_keys[17], 71), 0),
        "head_gain": jnp.clip(1.0 + 0.18 * jax.random.normal(arg_keys[8], (DV,), jnp.float32), 0.099609375, 1.8984375).astype(jnp.bfloat16),
        "residual": normal_values(arg_keys[9], (TOKENS, D), 1.0, 6.0, ((0, 32),)),
        "out_weight": normal_values(arg_keys[10], (2 * HG * DV, D), (2 * HG * DV) ** -0.5, 0.25),
        "norm_gains": jnp.clip(1.0 + 0.18 * jax.random.normal(arg_keys[11], (2, D), jnp.float32), 0.099609375, 1.8984375).astype(jnp.bfloat16),
        "routes": draw_routes(jax.random.fold_in(arg_keys[17], 71), 0),
        "route_weights": jnp.clip(0.1 + 0.9 * jax.random.uniform(arg_keys[13], (TOKENS, TOPK), jnp.float32) ** shard_levels(arg_keys[13], (TOKENS, TOPK), ((0, 32),), -0.2, 0.2), 0.1, 1.0),
        "gate_weight": normal_values(arg_keys[14], (EXPERTS, D, FF), D ** -0.5, 0.125, ((0, 16), (2, 2))),
        "up_weight": normal_values(arg_keys[15], (EXPERTS, D, FF), D ** -0.5, 0.125, ((0, 16), (2, 2))),
        "down_weight": normal_values(arg_keys[16], (EXPERTS, FF, D), FF ** -0.5, 0.1875, ((0, 16), (1, 2))),
    }


residual_gain = 8.0 ** 0.25
epsilon = 1e-05

def layer_norm(values, gain_row):
    average = lax.optimization_barrier(jnp.mean(values, axis=-1, keepdims=True))
    centred = values - average
    variance = lax.optimization_barrier(jnp.mean(centred * centred, axis=-1, keepdims=True))
    return centred * lax.rsqrt(variance + epsilon) * gain_row.astype(jnp.float32)

def group_attention(queries, keyset, valueset, lambda_row, slope_row, head_gain):
    length, head_count, doubled = queries.shape
    key_width = doubled // 2
    query_four = queries.reshape(length, head_count, 2, key_width).astype(jnp.float32)
    key_four = keyset.reshape(length, head_count, 2, key_width).astype(jnp.float32)
    value_all = valueset.astype(jnp.float32)
    block_rows = math.gcd(length, 512)
    key_places = jnp.arange(length, dtype=jnp.int32)

    def one_block(number):
        query_block = lax.dynamic_slice_in_dim(query_four, number * block_rows, block_rows, 0)
        query_places = number * block_rows + jnp.arange(block_rows, dtype=jnp.int32)
        distance = (query_places[:, None] - key_places[None, :]).astype(jnp.float32)
        scores = jnp.einsum('qhmd,khmd->hmqk', query_block, key_four) * key_width ** (-0.5)
        scores = scores - slope_row[:, None, None, None] * distance
        scores = jnp.where(distance >= 0, scores, -jnp.inf)
        highest = lax.optimization_barrier(jnp.max(scores, axis=-1, keepdims=True))
        exponent = jnp.exp(scores - highest)
        totals = lax.optimization_barrier(jnp.sum(exponent, axis=-1))
        rounded = lax.optimization_barrier(exponent.astype(jnp.bfloat16)).astype(jnp.float32)
        mixture = jnp.einsum('hmqk,khe->hmqe', rounded, value_all) / totals[..., None]
        head_out = mixture[:, 0] - lambda_row[:, None, None] * mixture[:, 1]
        scaled = head_out * lax.rsqrt(lax.optimization_barrier(jnp.mean(head_out * head_out, axis=-1, keepdims=True)) + epsilon)
        scaled = scaled * head_gain.astype(jnp.float32)
        return jnp.transpose(scaled, (1, 0, 2))
    blocks = lax.map(one_block, jnp.arange(length // block_rows, dtype=jnp.int32))
    return blocks.reshape(length, head_count, -1)

def expert_pass(middle, routes, route_weights, gate_weight, up_weight, down_weight):
    pair_ids = routes.reshape(-1).astype(jnp.int32)
    pair_count = pair_ids.shape[0]
    ordering = jnp.argsort(pair_ids, stable=True).astype(jnp.int32)
    counts = lax.optimization_barrier(jnp.sum((pair_ids[None, :] == jnp.arange(EXPERTS, dtype=jnp.int32)[:, None]).astype(jnp.int32), axis=1))
    starts = (jnp.cumsum(counts) - counts).astype(jnp.int32)
    most_rows = CAP * (TOKENS // ROWS)
    padded = jnp.concatenate([ordering, jnp.zeros((most_rows,), jnp.int32)])
    part_width = FF // N_TP
    features = middle.shape[1]

    def per_expert(collected, expert):
        slot_rows = lax.dynamic_slice_in_dim(padded, starts[expert], most_rows, 0)
        in_use = jnp.arange(most_rows, dtype=jnp.int32) < counts[expert]
        inputs = middle[slot_rows // 2]
        gate_in = jnp.dot(inputs, gate_weight[expert], preferred_element_type=jnp.float32)
        up_in = jnp.dot(inputs, up_weight[expert], preferred_element_type=jnp.float32)
        hidden = (jax.nn.silu(gate_in) * up_in).astype(jnp.bfloat16)
        summed = jnp.zeros((most_rows, features), jnp.float32)
        for number in range(N_TP):
            partial_value = jnp.dot(hidden[:, number * part_width:(number + 1) * part_width], down_weight[expert, number * part_width:(number + 1) * part_width], preferred_element_type=jnp.float32)
            summed = summed + lax.optimization_barrier(partial_value.astype(jnp.bfloat16)).astype(jnp.float32)
        result = lax.optimization_barrier(summed.astype(jnp.bfloat16)).astype(jnp.float32)
        collected = collected.at[slot_rows].add(jnp.where(in_use[:, None], result, 0.0))
        return (collected, None)
    pair_out, _ = lax.scan(per_expert, jnp.zeros((pair_count, features), jnp.float32), jnp.arange(EXPERTS, dtype=jnp.int32))
    weighted = route_weights.reshape(-1, 1) * pair_out
    return lax.optimization_barrier(jnp.sum(weighted.reshape(TOKENS, TOPK, features), axis=1))

def reference(query_small, key_small, value_small, query_large, key_large, value_large, lambdas, slopes, head_gain, residual, out_weight, norm_gains, routes, route_weights, gate_weight, up_weight, down_weight):
    small_out = group_attention(query_small, key_small, value_small, lambdas[:, 0], slopes[:, 0], head_gain)
    large_out = group_attention(query_large, key_large, value_large, lambdas[:, 1], slopes[:, 1], head_gain)
    attended = jnp.stack([small_out, large_out], axis=2).astype(jnp.bfloat16).reshape(TOKENS, -1)
    projected = jnp.dot(attended, out_weight, preferred_element_type=jnp.float32)
    middle = layer_norm(residual_gain * residual.astype(jnp.float32) + projected, norm_gains[0]).astype(jnp.bfloat16)
    moe_sum = expert_pass(middle, routes, route_weights, gate_weight, up_weight, down_weight)
    return layer_norm(residual_gain * middle.astype(jnp.float32) + moe_sum, norm_gains[1]).astype(jnp.bfloat16)
```

```python
import jax
import jax.numpy as jnp
from jax import lax
from jax.experimental import pallas as pl
from jax.experimental.pallas import tpu as pltpu
from jax.sharding import PartitionSpec as P

residual_gain = 8.0**0.25
epsilon = 1e-05
masked_score = -1e30
log2_e = 1.4426950408889634


def layer_norm(values, gain_row):
    average = jnp.mean(values, axis=-1, keepdims=True)
    centred = values - average
    variance = jnp.mean(centred * centred, axis=-1, keepdims=True)
    return centred * lax.rsqrt(variance + epsilon) * gain_row.astype(jnp.float32)


def attention_kernel(
    place, lambda_ref, slope_ref, gain_ref, small_ref, large_ref, block_ref, out_ref, bias, top, total, mixed
):
    step = pl.program_id(0)
    mine = place[0]
    length = small_ref.shape[0]
    rows = block_ref.shape[0]
    small = small_ref.shape[1] // 2
    large = large_ref.shape[1] // 2
    value = out_ref.shape[1] // 2
    small_value = 2 * small
    large_key = small_value + value
    large_value = large_key + 2 * large

    @pl.when(step == 0)
    def _():
        apart = lax.broadcasted_iota(jnp.int32, (rows, length), 0) - lax.broadcasted_iota(
            jnp.int32, (rows, length), 1
        )
        for group in range(2):
            bias[group] = apart.astype(jnp.float32) * (slope_ref[group] * log2_e)
        top[...] = jnp.full(top.shape, masked_score, jnp.float32)
        total[...] = jnp.zeros(total.shape, jnp.float32)
        mixed[...] = jnp.zeros(mixed.shape, jnp.float32)

    def fold(diagonal):
        for group in range(2):
            width = (small, large)[group]
            key_start = (0, large_key)[group]
            value_start = (small_value, large_value)[group]
            query_ref = (small_ref, large_ref)[group]
            values = block_ref[:, value_start : value_start + value]
            away = ((step - mine) * rows).astype(jnp.float32) * (slope_ref[group] * log2_e)
            for part in range(2):
                number = 2 * group + part
                keys = block_ref[:, key_start + part * width : key_start + (part + 1) * width]
                queries = query_ref[:, part * width : (part + 1) * width]
                scores = lax.dot_general(
                    keys, queries, (((1,), (1,)), ((), ())), preferred_element_type=jnp.float32
                )
                scores = scores * (width ** (-0.5) * log2_e) + bias[group]
                if diagonal:
                    seen = lax.broadcasted_iota(jnp.int32, (rows, length), 0)
                    asked = lax.broadcasted_iota(jnp.int32, (rows, length), 1)
                    scores = jnp.where(seen <= asked, scores, masked_score)
                old = top[number]
                new = jnp.maximum(old, jnp.max(scores, axis=0, keepdims=True) + away)
                weights = jnp.exp2(scores - (new - away))
                factor = jnp.exp2(old - new)
                top[number] = new
                total[number] = total[number] * factor + jnp.sum(weights, axis=0, keepdims=True)
                mixed[number] = mixed[number] * factor + lax.dot_general(
                    values,
                    weights.astype(jnp.bfloat16),
                    (((0,), (0,)), ((), ())),
                    preferred_element_type=jnp.float32,
                )

    @pl.when(step < mine)
    def _():
        fold(False)

    @pl.when(step == mine)
    def _():
        fold(True)
        for group in range(2):
            first = mixed[2 * group] / total[2 * group]
            second = mixed[2 * group + 1] / total[2 * group + 1]
            head_out = first - lambda_ref[group] * second
            square = jnp.mean(head_out * head_out, axis=0, keepdims=True)
            head_out = (head_out * lax.rsqrt(square + epsilon)).T
            out_ref[:, group * value : (group + 1) * value] = (
                head_out * gain_ref[...].astype(jnp.float32)
            ).astype(jnp.bfloat16)


def attend(place, lambda_row, slope_row, head_gain, small_queries, large_queries, gathered):
    length = small_queries.shape[0]
    value = head_gain.shape[0]
    columns = gathered.shape[1]
    whole = lambda step, place: (0, 0)
    return pl.pallas_call(
        attention_kernel,
        grid_spec=pltpu.PrefetchScalarGridSpec(
            num_scalar_prefetch=1,
            grid=(gathered.shape[0] // length,),
            in_specs=[
                pl.BlockSpec(memory_space=pltpu.SMEM),
                pl.BlockSpec(memory_space=pltpu.SMEM),
                pl.BlockSpec((1, value), whole),
                pl.BlockSpec(small_queries.shape, whole),
                pl.BlockSpec(large_queries.shape, whole),
                pl.BlockSpec((length, columns), lambda step, place: (jnp.minimum(step, place[0]), 0)),
            ],
            out_specs=pl.BlockSpec((length, 2 * value), whole),
            scratch_shapes=[
                pltpu.VMEM((2, length, length), jnp.float32),
                pltpu.VMEM((4, 1, length), jnp.float32),
                pltpu.VMEM((4, 1, length), jnp.float32),
                pltpu.VMEM((4, value, length), jnp.float32),
            ],
        ),
        out_shape=jax.ShapeDtypeStruct((length, 2 * value), jnp.bfloat16),
        compiler_params=pltpu.CompilerParams(dimension_semantics=("arbitrary",)),
    )(place, lambda_row, slope_row, head_gain.reshape(1, -1), small_queries, large_queries, gathered)


def expert_half(rows, gate, up, down):
    gate_in = jnp.dot(rows, gate, preferred_element_type=jnp.float32)
    upward = jnp.dot(rows, up, preferred_element_type=jnp.float32)
    hidden = (jax.nn.silu(gate_in) * upward).astype(jnp.bfloat16)
    return jnp.dot(hidden, down, preferred_element_type=jnp.float32).astype(jnp.bfloat16)


def shards(
    query_small,
    key_small,
    value_small,
    query_large,
    key_large,
    value_large,
    lambdas,
    slopes,
    head_gain,
    residual,
    out_weight,
    norm_gains,
    routes,
    route_weights,
    gate_weight,
    up_weight,
    down_weight,
):
    length = query_small.shape[0]
    own = jnp.concatenate(
        [array[:, 0] for array in (key_small, value_small, key_large, value_large)], axis=1
    )
    gathered = lax.all_gather(own, "sp", axis=0, tiled=True)
    place = jnp.reshape(lax.axis_index("sp"), (1,)).astype(jnp.int32)
    attended = attend(
        place, lambdas[0], slopes[0], head_gain, query_small[:, 0], query_large[:, 0], gathered
    )
    row_count = length // lax.axis_size("tp")
    core = lax.axis_index("tp")
    swap = ((0, 1), (1, 0))
    halves = attended.reshape(2, row_count, -1)
    kept = jnp.where(core == 0, halves[0], halves[1])
    taken = lax.ppermute(jnp.where(core == 0, halves[1], halves[0]), "tp", swap)
    flattened = jnp.concatenate(
        [jnp.where(core == 0, kept, taken), jnp.where(core == 0, taken, kept)], axis=1
    )
    projected = jnp.dot(flattened, out_weight, preferred_element_type=jnp.float32)
    middle = layer_norm(
        residual_gain * residual.astype(jnp.float32) + projected, norm_gains[0]
    ).astype(jnp.bfloat16)
    experts = lax.axis_size("sp")
    capacity = 4 * row_count // experts
    features = middle.shape[1]
    chosen = routes.reshape(-1)
    matches = (chosen[:, None] == jnp.arange(experts)[None, :]).astype(jnp.int32)
    earlier = jnp.cumsum(matches, axis=0) - matches
    target = chosen * capacity + jnp.sum(earlier * matches, axis=1)
    selector = jnp.any(
        target.reshape(row_count, 2)[None, :, :] == jnp.arange(experts * capacity)[:, None, None],
        axis=2,
    ).astype(jnp.bfloat16)
    outgoing = jnp.dot(selector, middle, preferred_element_type=jnp.float32).astype(jnp.bfloat16)
    outgoing = outgoing.reshape(experts, capacity, features)
    arrived = lax.all_to_all(outgoing, "sp", split_axis=0, concat_axis=0, tiled=True)
    arrived = arrived.reshape(-1, features)
    other = lax.ppermute(arrived, "tp", swap)
    joined_partial = [
        expert_half(rows, gate_weight[0], up_weight[0], down_weight[0]) for rows in (other, arrived)
    ]
    back = lax.ppermute(joined_partial[0], "tp", swap)
    summed = (joined_partial[1].astype(jnp.float32) + back.astype(jnp.float32)).astype(jnp.bfloat16)
    returned = lax.all_to_all(
        summed.reshape(experts, capacity, features), "sp", split_axis=0, concat_axis=0, tiled=True
    )
    expert_out = returned.reshape(experts * capacity, features)
    picked = jnp.take(expert_out, target, axis=0).reshape(row_count, 2, features)
    moe_sum = jnp.sum(route_weights[:, :, None] * picked.astype(jnp.float32), axis=1)
    return layer_norm(residual_gain * middle.astype(jnp.float32) + moe_sum, norm_gains[1]).astype(
        jnp.bfloat16
    )


def solution(mesh):
    placed = (
        P("sp", "tp", None),
        P("sp", "tp", None),
        P("sp", "tp", None),
        P("sp", "tp", None),
        P("sp", "tp", None),
        P("sp", "tp", None),
        P("tp", None),
        P("tp", None),
        P(),
        P(("sp", "tp"), None),
        P(),
        P(),
        P(("sp", "tp"), None),
        P(("sp", "tp"), None),
        P("sp", None, "tp"),
        P("sp", None, "tp"),
        P("sp", "tp", None),
    )
    return jax.shard_map(
        shards, mesh=mesh, in_specs=placed, out_specs=P(("sp", "tp"), None), check_vma=False
    )
```
